32 devices in a mesh: gr: 2 (over x), fs: 8 (over z, y), tp: 2 (over core).
Axes of the slice: x: 2, y: 2, z: 4, core: 2. Of those that a mesh axis runs over, the one named last changes fastest.
Arguments:
- tokens: bfloat16 [4, 2048, 2048], P(('gr', 'tp')), may hold values from -6 to 6
- gate_master: float32 [3, 2048, 7168], P(None, 'fs', ('gr', 'tp')), may hold values from -0.125 to 0.125
- up_master: float32 [3, 2048, 7168], P(None, 'fs', ('gr', 'tp')), may hold values from -0.125 to 0.125
- down_master: float32 [3, 7168, 2048], P(None, 'fs', ('gr', 'tp')), may hold values from -0.0625 to 0.0625
- norm_gain: float32 [2048], P('fs'), may hold values from 0.1 to 1.9
- route: int32 [4, 2048, 2], P(('gr', 'tp')), may hold values from 0 to 2, all different within a row
- route_weight: float32 [4, 2048, 2], P(('gr', 'tp')), may hold values from 0.05 to 1
Outputs:
- gate_out: bfloat16 [3, 2048, 7168], P(None, None, 'fs')
- up_out: bfloat16 [3, 2048, 7168], P(None, None, 'fs')
- down_out: bfloat16 [3, 7168, 2048], P(None, 'fs')
- mixed: bfloat16 [4, 2048, 2048], P(('gr', 'tp'), 'fs')
The draws below stay inside these ranges and needn't reach their ends.
Inputs may be any that keep to these rules, and one draw needn't show every extreme that they name: `route`: each token names two different experts; every expert is named by some token.
All inputs are finite; a program needn't handle non-finite values.
Results may differ from the reference program's by a relative error of at most 0.024.
Values may be sent and summed in bfloat16 or wider, within the bound.
A program may use at most 192 MiB of HBM per device.

```python
import math
import jax
import jax.numpy as jnp
from jax import lax

D = 2048
FF = 7168
EXPERTS = 3
ROWS = 2048
REQ = 4
N_FS = 8


def steps_of(rng, shape, shards, low, largest):
    level, own = 1.0, jax.random.fold_in(rng, 6)
    for position, blocks in shards:
        heights = jnp.exp(jax.random.uniform(jax.random.fold_in(own, position), (blocks,), jnp.float32, low / len(shards), largest / len(shards)))
        level = level * jnp.repeat(heights, shape[position] // blocks).reshape([-1 if axis == position else 1 for axis in range(len(shape))])
    return level


def choose_distinct(rng, rows, number_of, top, lift):
    sequence = jax.random.permutation(jax.random.fold_in(rng, 1), number_of)
    boost = sequence
    for power in range(3):
        boost = boost * boost // number_of
    boost = boost * lift // number_of
    lots = jax.random.randint(jax.random.fold_in(rng, 2), (rows, number_of), 0, 4096) + boost
    holders = jax.random.permutation(jax.random.fold_in(rng, 3), rows)[jnp.arange(number_of) % rows]
    lots = jnp.where(jnp.arange(rows)[:, None] == holders[None, :], 1 << 14, lots)
    score = lots * number_of + jnp.arange(number_of)
    return lax.top_k(score.astype(jnp.int32), top)[1].astype(jnp.int32)


def gaussian(own_key, dims, spread, bound, split=(), held_as=jnp.bfloat16):
    values = jax.random.normal(own_key, dims, jnp.float32) * spread
    if len(split) > 0:
        values = steps_of(own_key, dims, split, -0.22, 0.18) * values
    return jnp.clip(values, min=-bound, max=bound).astype(held_as)


def setup_inputs(seed: int = 0) -> dict:
    seeds = jax.random.split(jax.random.key(seed), 8)
    tokens = gaussian(seeds[0], (REQ, ROWS, D), 1.0, 6.0, ((0, 4),))
    gate_master = gaussian(seeds[1], (EXPERTS, D, FF), D ** -0.5, 0.125, ((1, 8), (2, 4)), jnp.float32)
    up_master = gaussian(seeds[2], (EXPERTS, D, FF), D ** -0.5, 0.125, ((1, 8), (2, 4)), jnp.float32)
    down_master = gaussian(seeds[3], (EXPERTS, FF, D), FF ** -0.5, 0.0625, ((1, 8), (2, 4)), jnp.float32)
    norm_gain = jnp.clip(1.0 + 0.18 * jax.random.normal(seeds[4], (D,), jnp.float32), 0.1, 1.9)
    route = choose_distinct(seeds[5], REQ * ROWS, EXPERTS, 2, 0).reshape((REQ, ROWS, 2))
    route_weight = jnp.clip(jnp.exp(math.log(1.0) - 2.9957323 * jax.random.uniform(seeds[6], (REQ, ROWS, 2), jnp.float32) ** steps_of(seeds[6], (REQ, ROWS, 2), ((0, 4),), -0.2, 0.2)), 0.05, 1.0)
    return {"tokens": tokens, "gate_master": gate_master, "up_master": up_master, "down_master": down_master, "norm_gain": norm_gain, "route": route, "route_weight": route_weight}


def normalize(rows_in):
    values = rows_in.astype(jnp.float32)
    scaled = values * lax.rsqrt(lax.optimization_barrier(jnp.mean(values * values, axis=-1, keepdims=True)) + 1e-06)
    return scaled.astype(jnp.bfloat16)

def mixing(chosen, weights):
    share = weights / lax.optimization_barrier(jnp.sum(weights, axis=-1, keepdims=True))
    labels = jnp.arange(EXPERTS, dtype=jnp.int32)
    match = (chosen[:, :, None] == labels[None, None, :]).astype(jnp.float32)
    return lax.optimization_barrier(jnp.sum(share[:, :, None] * match, axis=1))

def reference(tokens, gate_master, up_master, down_master, norm_gain, route, route_weight):
    scaled_gain = norm_gain[None, :, None]
    gate_out = (scaled_gain * gate_master).astype(jnp.bfloat16)
    up_out = (scaled_gain * up_master).astype(jnp.bfloat16)
    down_out = down_master.astype(jnp.bfloat16)
    block_width = FF // N_FS

    def one_batch(batch):
        rows_in, chosen, weights = batch
        normed = normalize(rows_in)
        combine = mixing(chosen, weights)
        hidden_list = []
        for index in range(EXPERTS):
            gate_act = jnp.dot(normed, gate_out[index], preferred_element_type=jnp.float32)
            up_act = jnp.dot(normed, up_out[index], preferred_element_type=jnp.float32)
            hidden_list.append((jax.nn.silu(gate_act) * up_act).astype(jnp.bfloat16))

        def add_block(block, total):
            start = (block * block_width).astype(jnp.int32)
            partial_sum = jnp.zeros((rows_in.shape[0], rows_in.shape[1]), jnp.float32)
            for index in range(EXPERTS):
                hidden_part = lax.dynamic_slice_in_dim(hidden_list[index], start, block_width, 1)
                down_part = lax.dynamic_slice_in_dim(down_out[index], start, block_width, 0)
                projected = jnp.dot(hidden_part, down_part, preferred_element_type=jnp.float32)
                partial_sum = partial_sum + combine[:, index:index + 1] * projected
            return total + partial_sum.astype(jnp.bfloat16).astype(jnp.float32)
        total = lax.fori_loop(0, N_FS, add_block, jnp.zeros((rows_in.shape[0], rows_in.shape[1]), jnp.float32))
        return total.astype(jnp.bfloat16)
    mixed = lax.map(one_batch, (tokens, route, route_weight))
    return (gate_out, up_out, down_out, mixed)
```

```python
import jax
import jax.numpy as jnp
from jax import lax
from jax.sharding import PartitionSpec as P

CHUNKS = 2
GROUP = ("gr", "tp")


def normalize(rows_in):
    values = rows_in.astype(jnp.float32)
    scaled = values * lax.rsqrt(jnp.mean(values * values, axis=-1, keepdims=True) + 1e-06)
    return scaled.astype(jnp.bfloat16)


def mixing(chosen, weights, experts):
    share = weights / jnp.sum(weights, axis=-1, keepdims=True)
    labels = jnp.arange(experts, dtype=jnp.int32)
    match = (chosen[:, :, None] == labels[None, None, :]).astype(jnp.float32)
    return jnp.sum(share[:, :, None] * match, axis=1)


def expert_term(normed, mix_column, gate_weight, up_weight, down_weight):
    gate_act = jnp.dot(normed, gate_weight, preferred_element_type=jnp.float32)
    up_act = jnp.dot(normed, up_weight, preferred_element_type=jnp.float32)
    hidden = (jax.nn.silu(gate_act) * up_act).astype(jnp.bfloat16)
    projected = jnp.dot(hidden, down_weight, preferred_element_type=jnp.float32)
    return mix_column * projected


def make_shards(n_fs, n_group):
    def by_chunks(rows):
        parts = rows.reshape(n_fs, CHUNKS, -1, rows.shape[-1])
        return parts.transpose(1, 0, 2, 3).reshape(rows.shape)

    def shards(tokens, gate_master, up_master, down_master, norm_gain, route, route_weight):
        experts, depth, columns = gate_master.shape
        blocks = n_fs // n_group
        width = columns // blocks
        rows = depth // n_group

        down_local = down_master.astype(jnp.bfloat16)
        down_local, gate_master, up_master = lax.optimization_barrier((down_local, gate_master, up_master))
        down_list = [lax.all_gather(down_local[index], GROUP, axis=1, tiled=True) for index in range(experts)]

        def local(master, index):
            scaled = (norm_gain[:, None] * master[index]).astype(jnp.bfloat16)
            return scaled.reshape(n_group, rows, blocks, width).transpose(0, 2, 1, 3)

        me = lax.axis_index("fs")

        def permuted(sent):
            got = [lax.dynamic_index_in_dim(sent, me, 0, keepdims=True)]
            for shift in range(1, n_fs):
                block = lax.dynamic_index_in_dim(sent, lax.rem(me + shift, n_fs), 0, keepdims=True)
                got.append(lax.ppermute(block, "fs", [(i, (i + shift) % n_fs) for i in range(n_fs)]))
            return got

        def gathered(got):
            mine = jnp.zeros((n_fs,) + got[0].shape[1:], got[0].dtype)
            for shift in range(n_fs):
                source = lax.rem(me - shift + n_fs, n_fs)
                mine = lax.dynamic_update_slice_in_dim(mine, got[shift], source, 0)
            return tuple(
                lax.all_gather(mine[:, which], GROUP, axis=1, tiled=True).reshape(n_fs * depth, width)
                for which in range(2)
            )

        pair = jnp.stack([local(m, i) for i in range(experts) for m in (gate_master, up_master)], axis=2)
        pair = lax.all_to_all(pair, GROUP, split_axis=0, concat_axis=0, tiled=True)
        pair = pair.reshape(n_fs, 2 * experts, rows, width)

        got = [permuted(pair[:, 2 * index : 2 * index + 2]) for index in range(experts)]
        got[0], down_list = lax.optimization_barrier((got[0], down_list))

        normed = by_chunks(normalize(tokens[0]))
        combine = by_chunks(mixing(route[0], route_weight[0], experts))
        total = jnp.zeros(normed.shape, jnp.float32)
        weights = [gathered(got[index]) for index in range(min(2, experts))]
        for index in range(experts - 1):
            total = total + expert_term(
                normed, combine[:, index : index + 1], *weights[index], down_list[index]
            )
            if index + 2 < experts:
                got[index + 2], total = lax.optimization_barrier((got[index + 2], total))
                weights.append(gathered(got[index + 2]))
        last = experts - 1
        size = normed.shape[0] // CHUNKS
        mixed = []
        for chunk in range(CHUNKS):
            part = slice(chunk * size, (chunk + 1) * size)
            summed = total[part] + expert_term(
                normed[part], combine[part, last : last + 1], *weights[last], down_list[last]
            )
            summed = summed.astype(jnp.bfloat16)
            mixed.append(lax.psum_scatter(summed, "fs", scatter_dimension=0, tiled=True))
        weights, down_list, _ = lax.optimization_barrier((weights, down_list, summed))
        gate_out = jnp.stack([pair[0] for pair in weights], axis=0)
        up_out = jnp.stack([pair[1] for pair in weights], axis=0)
        down_out = jnp.stack(down_list, axis=0)
        return (gate_out, up_out, down_out, jnp.concatenate(mixed, axis=0)[None])

    return shards


def solution(mesh):
    n_fs = mesh.shape["fs"]
    n_group = mesh.shape["gr"] * mesh.shape["tp"]
    in_specs = (
        P(GROUP, None, None),
        P(None, "fs", GROUP),
        P(None, "fs", GROUP),
        P(None, "fs", GROUP),
        P("fs"),
        P(GROUP, None, None),
        P(GROUP, None, None),
    )
    out_specs = (
        P(None, None, "fs"),
        P(None, None, "fs"),
        P(None, "fs", None),
        P(GROUP, "fs", None),
    )
    return jax.shard_map(
        make_shards(n_fs, n_group), mesh=mesh, in_specs=in_specs, out_specs=out_specs, check_vma=False
    )
```
